32 devices in a mesh: sp: 4 (over y, core), tp: 8 (over z, x).
Axes of the slice: x: 2, y: 2, z: 4, core: 2. Of those that a mesh axis runs over, the one named last changes fastest.
Arguments:
- queries: bfloat16 [512, 3072], P('sp'), may hold values from -6 to 6
- attn_out: bfloat16 [512, 3072], P('sp'), may hold values from -3 to 3
- log_norm: float32 [512, 12], P('sp'), as said below
- cotangent: bfloat16 [512, 3072], P('sp'), may hold values from -96 to 96
- keys: bfloat16 [1024, 512], P(('sp', 'tp')), may hold values from -6 to 6
- values: bfloat16 [1024, 512], P(('sp', 'tp')), may hold values from -6 to 6
- source: bfloat16 [1024, 3072], P('sp', 'tp'), may hold values from -6 to 6
- w_query: bfloat16 [3072, 3072], P('tp'), may hold values from -0.109375 to 0.109375
- w_key: bfloat16 [3072, 512], P('tp'), may hold values from -0.109375 to 0.109375
- w_value: bfloat16 [3072, 512], P('tp'), may hold values from -0.109375 to 0.109375
Outputs:
- d_target: bfloat16 [512, 3072], P('sp', 'tp')
- d_source: bfloat16 [1024, 3072], P('sp', 'tp')
- d_wvalue: float32 [3072, 512], P('tp')
The draws below stay inside these ranges and needn't reach their ends.
Inputs may be any that keep to these rules, and one draw needn't show every extreme that they name: `log_norm`: the logarithm of the softmax total saved by the forward pass, near log(1024) + 0.5.
All inputs are finite; a program needn't handle non-finite values.
Results may differ from the reference program's by a relative error of at most 0.024.
Values may be sent and summed in bfloat16 or wider, within the bound.
A program may use at most 64 MiB of HBM per device.

```python
import math
import jax
import jax.numpy as jnp
from jax import lax

HEADS = 12
KV_HEADS = 2
HEAD_DIM = 256
TARGET_ROWS_EACH = 128
D = 3072
KW = 512
TGT = 512
SRC = 1024


def draw_log_norm(key, part):
    center = math.log(SRC) + 0.5
    spread = jax.random.uniform(key, (TGT, HEADS), jnp.float32, -0.5, 0.5)
    return (center + spread).astype(jnp.float32)


def level_of(key, dims, cuts, low, largest):
    def one(dim, blocks):
        heights = jax.random.uniform(jax.random.fold_in(jax.random.fold_in(key, 6), dim), (blocks,), jnp.float32, low / len(cuts), largest / len(cuts))
        return jnp.repeat(jnp.exp(heights), dims[dim] // blocks).reshape((-1,) + (1,) * (len(dims) - dim - 1))

    level = one(*cuts[0])
    for cut in cuts[1:]:
        level = level * one(*cut)
    return level


def scatter_about(own_key, extent, deviation, limit, shards=(), kind=jnp.bfloat16):
    factor_of = level_of(own_key, extent, shards, -0.22, 0.18) if shards else 1.0
    values = jax.random.normal(own_key, extent, jnp.float32) * deviation * factor_of
    return jnp.minimum(jnp.maximum(values, -limit), limit).astype(kind)


def setup_inputs(seed: int = 0) -> dict:
    splits = jax.random.split(jax.random.key(seed), 11)
    return {
        "queries": scatter_about(splits[0], (TGT, D), 1.0, 6.0, ((0, 4),)),
        "attn_out": scatter_about(splits[1], (TGT, D), 0.5, 3.0, ((0, 4),)),
        "log_norm": draw_log_norm(jax.random.fold_in(splits[10], 71), 0),
        "cotangent": scatter_about(splits[3], (TGT, D), 16.0, 96.0, ((0, 4),)),
        "keys": scatter_about(splits[4], (SRC, KW), 1.0, 6.0, ((0, 32),)),
        "values": scatter_about(splits[5], (SRC, KW), 1.0, 6.0, ((0, 32),)),
        "source": scatter_about(splits[6], (SRC, D), 1.0, 6.0, ((0, 4), (1, 8))),
        "w_query": scatter_about(splits[7], (D, D), D ** -0.5, 0.109375, ((0, 8),)),
        "w_key": scatter_about(splits[8], (D, KW), D ** -0.5, 0.109375, ((0, 8),)),
        "w_value": scatter_about(splits[9], (D, KW), D ** -0.5, 0.109375, ((0, 8),)),
    }


def reference(queries, attn_out, log_norm, cotangent, keys, values, source, w_query, w_key, w_value):
    single_precision = jnp.float32
    repeat = HEADS // KV_HEADS
    score_scale = 1.0 / math.sqrt(HEAD_DIM)
    src_rows = keys.shape[0]
    shared_key_heads = keys.astype(single_precision).reshape(src_rows, KV_HEADS, HEAD_DIM)
    shared_value_heads = values.astype(single_precision).reshape(src_rows, KV_HEADS, HEAD_DIM)
    blocks = queries.shape[0] // TARGET_ROWS_EACH

    def step(carry, index):
        dk_total, dv_total = carry
        start = index * TARGET_ROWS_EACH

        def rows(array):
            return lax.dynamic_slice_in_dim(array, start, TARGET_ROWS_EACH, 0)
        query_tensor4 = rows(queries).astype(single_precision).reshape(TARGET_ROWS_EACH, KV_HEADS, repeat, HEAD_DIM)
        output_gradient4 = rows(cotangent).astype(single_precision).reshape(TARGET_ROWS_EACH, KV_HEADS, repeat, HEAD_DIM)
        out4 = rows(attn_out).astype(single_precision).reshape(TARGET_ROWS_EACH, KV_HEADS, repeat, HEAD_DIM)
        lse = jnp.transpose(rows(log_norm).reshape(TARGET_ROWS_EACH, KV_HEADS, repeat), (1, 2, 0))[..., None]
        delta = jnp.transpose(lax.optimization_barrier(jnp.sum(output_gradient4 * out4, axis=3)), (1, 2, 0))[..., None]
        logit_scores = jnp.einsum('znjk,wnk->njzw', query_tensor4, shared_key_heads) * score_scale
        probs = jnp.exp(logit_scores - lse)
        probabilities16 = lax.optimization_barrier(probs.astype(jnp.bfloat16)).astype(single_precision)
        prob_gradient = jnp.einsum('znjk,wnk->njzw', output_gradient4, shared_value_heads)
        score_gradient = lax.optimization_barrier((probs * (prob_gradient - delta)).astype(jnp.bfloat16)).astype(single_precision)
        query_gradient = (jnp.einsum('wohn,nwb->hwob', score_gradient, shared_key_heads) * score_scale).reshape(TARGET_ROWS_EACH, -1)
        key_gradient = jnp.einsum('nkjv,jnka->vna', score_gradient, query_tensor4) * score_scale
        value_gradient = jnp.einsum('nkjv,jnka->vna', probabilities16, output_gradient4)
        dk16 = lax.optimization_barrier(key_gradient.reshape(src_rows, -1).astype(jnp.bfloat16)).astype(single_precision)
        dv16 = lax.optimization_barrier(value_gradient.reshape(src_rows, -1).astype(jnp.bfloat16)).astype(single_precision)
        return ((dk_total + dk16, dv_total + dv16), query_gradient.astype(jnp.bfloat16))
    start_carry = (jnp.zeros((src_rows, KW), single_precision), jnp.zeros((src_rows, KW), single_precision))
    (dk_total, dv_total), dq_blocks = lax.scan(step, start_carry, jnp.arange(blocks, dtype=jnp.int32))
    dq16 = dq_blocks.reshape(queries.shape[0], -1)
    d_target = jnp.dot(dq16, w_query.T, preferred_element_type=single_precision).astype(jnp.bfloat16)
    stacked = jnp.concatenate([dk_total.astype(jnp.bfloat16), dv_total.astype(jnp.bfloat16)], axis=1)
    weights = jnp.concatenate([w_key, w_value], axis=1)
    d_source = jnp.dot(stacked, weights.T, preferred_element_type=single_precision).astype(jnp.bfloat16)
    d_wvalue = jnp.dot(source.T, dv_total.astype(jnp.bfloat16), preferred_element_type=single_precision)
    return (d_target, d_source, d_wvalue)
```

```python
import functools
import math

import jax
import jax.numpy as jnp
from jax import lax
from jax.experimental import pallas as pl
from jax.experimental.pallas import tpu as pltpu
from jax.sharding import PartitionSpec as P

HEADS = 12
KV_HEADS = 2
HEAD_DIM = 256
CORES = 2
SIDE = 2
VMEM_BYTES = 60 * 1024 * 1024
MESH = pl.DeviceIdType.MESH
NT = (((1,), (1,)), ((), ()))
TN = (((0,), (0,)), ((), ()))
F32 = jnp.float32
BF16 = jnp.bfloat16


def dot(a, b, dims=(((1,), (0,)), ((), ()))):
    return lax.dot_general(a, b, dims, preferred_element_type=F32)


def kernel(
    sp, tp, lse_ref, k_ref, v_ref, q_hbm, o_hbm, do_hbm, src_hbm, wq_hbm, wk_hbm, wv_hbm,
    dt_ref, ds_ref, dw_ref,
    kv, qs, dos, os_, wq, wk, wv, src, lse, delta, dqa, dq16, part, got, full,
    load_sem, near_send, near_recv, kv_send, kv_recv, kv_pair_send, kv_pair_recv,
    src_send, src_recv, part_send, part_recv, g_send, g_recv, gy_send, gy_recv, gp_send, gp_recv,
):
    rows = q_hbm.shape[0]
    rs, kw = k_ref.shape
    repeat = HEADS // KV_HEADS
    scale = 1.0 / math.sqrt(HEAD_DIM)
    i, j = lax.axis_index("sp"), lax.axis_index("tp")
    ny, nz = sp // CORES, tp // SIDE
    y, c = i // CORES, lax.rem(i, CORES)
    z, x = j // SIDE, lax.rem(j, SIDE)
    sp_peers = [lax.rem(i + k, sp) for k in range(1, sp)]
    y_peers = [lax.rem(y + k, ny) * CORES + c for k in range(1, ny)]
    pair = y * CORES + 1 - c
    zs = [lax.rem(z + k, nz) for k in range(1, nz)]
    z_peers = [a * SIDE + x for a in zs]
    jx = z * SIDE + 1 - x
    sends = []

    def send(ref_from, ref_to, s, r, device):
        copy = pltpu.make_async_remote_copy(
            src_ref=ref_from, dst_ref=ref_to, send_sem=s, recv_sem=r,
            device_id=device, device_id_type=MESH,
        )
        copy.start()
        sends.append(copy)

    def receive(ref, r):
        pltpu.make_async_remote_copy(
            src_ref=ref, dst_ref=ref, send_sem=load_sem.at[0], recv_sem=r,
            device_id=(pair, j), device_id_type=MESH,
        ).wait_recv()

    loads = []

    def load(ref_from, ref_to):
        copy = pltpu.make_async_copy(ref_from, ref_to, load_sem.at[len(loads)])
        copy.start()
        loads.append(copy)
        return copy

    barrier = pltpu.get_barrier_semaphore()
    near = [(p, j) for p in sp_peers] + [(i, p) for p in z_peers] + [(i, jx)]
    for d in near:
        pl.semaphore_signal(barrier, inc=1, device_id=d, device_id_type=MESH)
    near_rows = pl.ds(pl.multiple_of(i * rs, rs), rs)
    own_copies = [load(r, kv.at[t, j, near_rows]) for t, r in enumerate((k_ref, v_ref))]
    attn_loads = []
    for g in range(KV_HEADS):
        for h in range(repeat):
            columns = pl.ds((g * repeat + h) * HEAD_DIM, HEAD_DIM)
            for a, b in ((q_hbm, qs), (do_hbm, dos), (o_hbm, os_)):
                attn_loads.append(load(a.at[:, columns], b.at[g, pl.ds(h * rows, rows)]))
    src_load = load(src_hbm, src.at[i])
    weight_loads = [load(wq_hbm, wq), load(wk_hbm, wk), load(wv_hbm, wv)]
    pl.semaphore_wait(barrier, len(near))

    for n, p in enumerate(sp_peers):
        for t, r in enumerate((k_ref, v_ref)):
            send(r, kv.at[t, j, near_rows], near_send.at[t, n], near_recv.at[t, i], (p, j))

    src_load.wait()
    for n, p in enumerate(y_peers):
        send(src.at[i], src.at[i], src_send.at[n], src_recv.at[i], (p, j))
    send(src.at[i], src.at[i], src_send.at[ny], src_recv.at[i], (pair, j))

    for copy in attn_loads:
        copy.wait()
    for g in range(KV_HEADS):
        for h in range(repeat):
            at = pl.ds(h * rows, rows)
            d = jnp.sum(dos[g, at].astype(F32) * os_[g, at].astype(F32), axis=1, keepdims=True)
            delta[g, at] = jnp.broadcast_to(d, (rows, 128))
            n = g * repeat + h
            lse[g, at] = jnp.broadcast_to(lse_ref[:, n:n + 1], (rows, 128))

    for copy in own_copies:
        copy.wait()
    for p in sp_peers:
        for t in range(2):
            receive(kv.at[t, j, pl.ds(pl.multiple_of(p * rs, rs), rs)], near_recv.at[t, p])

    def kv_to_x(slot, n):
        send(kv.at[c, slot], kv.at[c, slot], kv_send.at[n], kv_recv.at[slot], (i, jx))

    def kv_to_pair(slot):
        send(kv.at[c, slot], kv.at[c, slot], kv_pair_send.at[slot], kv_pair_recv.at[slot], (pair, j))

    kv_to_x(j, 0)
    for n, p in enumerate(z_peers):
        send(kv.at[c, j], kv.at[c, j], kv_send.at[nz + n], kv_recv.at[j], (i, p))

    def wide(a, n):
        return a if n == 1 else jnp.concatenate([a] * n, axis=1)

    def grads(g, keys, values):
        n = keys.shape[0] // 128
        p = jnp.exp(dot(qs[g], keys, NT) * scale - wide(lse[g], n))
        dp = dot(dos[g], values, NT)
        ds = (p * (dp - wide(delta[g], n))).astype(BF16)
        return p, ds

    def head_columns(g):
        return slice(g * HEAD_DIM, (g + 1) * HEAD_DIM)

    for g in range(KV_HEADS):
        cols = head_columns(g)
        keys = kv[0, j, :, cols]
        p, ds = grads(g, keys, kv[1, j, :, cols])
        dk = dot(ds, qs[g], TN) * scale
        dv = dot(p.astype(BF16), dos[g], TN)
        part[:, 0, :, cols] = dk.astype(BF16).reshape(sp, rs, HEAD_DIM)
        part[:, 1, :, cols] = dv.astype(BF16).reshape(sp, rs, HEAD_DIM)
        dqa[g] = dot(ds, keys)
    for n, p in enumerate(sp_peers):
        send(part.at[p], got.at[i], part_send.at[n], part_recv.at[i], (p, j))

    def chunk_one(slot):
        for g in range(KV_HEADS):
            cols = head_columns(g)
            keys = kv[0, slot, :, cols]
            _, ds = grads(g, keys, kv[1, slot, :, cols])
            dqa[g] += dot(ds, keys)

    def chunk_z(a):
        slots = pl.ds(a * SIDE, SIDE)
        for g in range(KV_HEADS):
            cols = head_columns(g)
            keys = kv[0, slots, :, cols].reshape(-1, HEAD_DIM)
            values = kv[1, slots, :, cols].reshape(-1, HEAD_DIM)
            _, ds = grads(g, keys, values)
            dqa[g] += dot(ds, keys)

    def from_z(n):
        slot = z_peers[n]
        receive(kv.at[c, slot], kv_recv.at[slot])
        kv_to_x(slot, n + 1)
        kv_to_pair(slot)

    def from_x(slot):
        receive(kv.at[c, slot], kv_recv.at[slot])
        kv_to_pair(slot)

    def from_pair(slot):
        receive(kv.at[1 - c, slot], kv_pair_recv.at[slot])

    def g_to_x(slot, n):
        send(full.at[i, slot], full.at[i, slot], g_send.at[n], g_recv.at[slot], (i, jx))

    def g_spread(slot):
        for n, p in enumerate(y_peers):
            send(full.at[i, slot, 1], full.at[i, slot, 1], gy_send.at[n, slot], gy_recv.at[i, slot], (p, j))
        send(full.at[i, slot, 1], full.at[i, slot, 1], gp_send.at[i, slot], gp_recv.at[i, slot], (pair, j))

    def g_from_z(n):
        slot = z_peers[n]
        receive(full.at[i, slot], g_recv.at[slot])
        g_to_x(slot, n + 1)
        g_spread(slot)

    def g_from_x(slot):
        receive(full.at[i, slot], g_recv.at[slot])
        g_spread(slot)

    def g_from_y(slot):
        for p in y_peers:
            receive(full.at[p, slot, 1], gy_recv.at[p, slot])
            send(full.at[p, slot, 1], full.at[p, slot, 1], gp_send.at[p, slot], gp_recv.at[p, slot], (pair, j))

    from_x(jx)
    from_z(0)
    for n, p in enumerate(y_peers):
        receive(src.at[p], src_recv.at[p])
        send(src.at[p], src.at[p], src_send.at[ny + 1 + n], src_recv.at[p], (pair, j))
    from_pair(jx)
    chunk_one(jx)

    total = part[i].astype(F32)
    for p in sp_peers:
        receive(got.at[p], part_recv.at[p])
        total += got[p].astype(F32)
    full[i, j] = total.astype(BF16)
    for n in range(1, nz - 2):
        from_z(n)
    g_to_x(j, 0)
    for n, p in enumerate(z_peers):
        send(full.at[i, j], full.at[i, j], g_send.at[nz + n], g_recv.at[j], (i, p))
    g_spread(j)
    far = [a * SIDE + 1 - x for a in zs]
    from_x(far[0])
    from_pair(z_peers[0])
    from_pair(far[0])
    chunk_z(zs[0])
    for n in range(nz - 1):
        if n == 1:
            from_z(nz - 2)
            from_x(far[1])
            from_pair(z_peers[1])
            from_pair(far[1])
            chunk_z(zs[1])
        g_from_z(n)
        if n == 0:
            g_from_x(jx)
            g_from_y(j)
    for n in range(2, nz - 1):
        from_x(far[n])
        from_pair(z_peers[n])
        from_pair(far[n])
        chunk_z(zs[n])
    for n in range(nz - 1):
        g_from_x(far[n])
    for copy in weight_loads:
        copy.wait()
    for g in range(KV_HEADS):
        for h in range(repeat):
            n = g * repeat + h
            dq16[:, n * HEAD_DIM:(n + 1) * HEAD_DIM] = (dqa[g, h * rows:(h + 1) * rows] * scale).astype(BF16)
    dt_ref[...] = dot(dq16[...], wq[...], NT).astype(BF16)
    for slot in [jx] + z_peers + far:
        g_from_y(slot)
    ds_ref[...] = (
        dot(full[i, :, 0].reshape(-1, kw), wk[...], NT) + dot(full[i, :, 1].reshape(-1, kw), wv[...], NT)
    ).astype(BF16)
    theirs = [lax.rem(y + k, ny) * CORES + 1 - c for k in range(ny)]
    for p in theirs:
        receive(src.at[p], src_recv.at[p])
        for slot in range(tp):
            receive(full.at[p, slot, 1], gp_recv.at[p, slot])
    dw = dot(src[0], full[0, :, 1].reshape(-1, kw), TN)
    for b in range(1, sp):
        dw += dot(src[b], full[b, :, 1].reshape(-1, kw), TN)
    dw_ref[...] = dw
    for copy in sends:
        copy.wait_send()


def fused(sp, tp, scratch, queries, attn_out, log_norm, cotangent, keys, values, source, w_query, w_key, w_value):
    rows = queries.shape[0]
    width = w_value.shape[0]
    vmem, hbm = pl.BlockSpec(memory_space=pltpu.VMEM), pl.BlockSpec(memory_space=pl.ANY)
    dma = pltpu.SemaphoreType.DMA
    nz, ny = tp // SIDE, sp // CORES
    return pl.pallas_call(
        functools.partial(kernel, sp, tp),
        out_shape=(
            jax.ShapeDtypeStruct((rows, width), BF16),
            jax.ShapeDtypeStruct((source.shape[0], width), BF16),
            jax.ShapeDtypeStruct(w_value.shape, F32),
        ),
        in_specs=[vmem] * 3 + [hbm] * 7,
        out_specs=(vmem,) * 3,
        scratch_shapes=[pltpu.VMEM(s, t) for s, t in scratch] + [
            dma((3 * HEADS + 6,)), dma((2, sp)), dma((2, sp)), dma((2 * nz,)), dma((tp,)), dma((tp,)), dma((tp,)),
            dma((2 * ny,)), dma((sp,)), dma((sp,)), dma((sp,)), dma((2 * nz,)), dma((tp,)),
            dma((ny, tp)), dma((sp, tp)), dma((sp, tp)), dma((sp, tp)),
        ],
        compiler_params=pltpu.CompilerParams(
            collective_id=0, has_side_effects=True, vmem_limit_bytes=VMEM_BYTES
        ),
    )(log_norm, keys, values, queries, attn_out, cotangent, source, w_query, w_key, w_value)


def scratch_of(sp, tp, queries, keys, source, w_query, w_value):
    rows, width = queries.shape
    rs, kw = keys.shape
    stack = (KV_HEADS, rows * HEADS // KV_HEADS, HEAD_DIM)
    flat = stack[:2] + (128,)
    return [
        ((2, tp, sp * rs, kw), BF16), (stack, BF16), (stack, BF16), (stack, BF16),
        (w_query.shape, BF16), (w_value.shape, BF16), (w_value.shape, BF16),
        ((sp,) + source.shape, BF16), (flat, F32), (flat, F32), (stack, F32), ((rows, width), BF16),
        ((sp, 2, rs, kw), BF16), ((sp, 2, rs, kw), BF16), ((sp, tp, 2, rs, kw), BF16),
    ]


def shards(sp, tp, *args):
    queries, _, _, _, keys, _, source, w_query, _, w_value = args
    scratch = scratch_of(sp, tp, queries, keys, source, w_query, w_value)
    size = sum(math.prod(s) * jnp.dtype(t).itemsize for s, t in scratch)
    fits = size * 2 < VMEM_BYTES and sp * keys.shape[0] == 128
    if fits and sp % CORES == 0 and tp == 4 * SIDE:
        return fused(sp, tp, scratch, *args)
    return plain(*args)


def plain(queries, attn_out, log_norm, cotangent, keys, values, source, w_query, w_key, w_value):
    single_precision = jnp.float32
    repeat = HEADS // KV_HEADS
    score_scale = 1.0 / math.sqrt(HEAD_DIM)
    rows = queries.shape[0]
    near_keys, near_values = (
        lax.all_gather(keys, "sp", axis=0, tiled=True),
        lax.all_gather(values, "sp", axis=0, tiled=True),
    )
    span = near_keys.shape[0]
    query_tensor4 = queries.reshape(rows, KV_HEADS, repeat, HEAD_DIM)
    output_gradient4 = cotangent.reshape(rows, KV_HEADS, repeat, HEAD_DIM)
    out4 = attn_out.reshape(rows, KV_HEADS, repeat, HEAD_DIM)
    shared_key_heads = near_keys.reshape(span, KV_HEADS, HEAD_DIM)
    shared_value_heads = near_values.reshape(span, KV_HEADS, HEAD_DIM)
    delta = jnp.sum(
        output_gradient4.astype(single_precision) * out4.astype(single_precision), axis=3
    )
    delta = jnp.transpose(delta, (1, 2, 0))[..., None]
    lse = jnp.transpose(log_norm.reshape(rows, KV_HEADS, repeat), (1, 2, 0))[..., None]
    logit_scores = (
        jnp.einsum(
            "znjk,wnk->njzw",
            query_tensor4,
            shared_key_heads,
            preferred_element_type=single_precision,
        )
        * score_scale
    )
    probs = jnp.exp(logit_scores - lse)
    probabilities16 = probs.astype(jnp.bfloat16)
    prob_gradient = jnp.einsum(
        "znjk,wnk->njzw",
        output_gradient4,
        shared_value_heads,
        preferred_element_type=single_precision,
    )
    score_gradient = (probs * (prob_gradient - delta)).astype(jnp.bfloat16)
    query_gradient_piece = (
        jnp.einsum(
            "wohn,nwb->hwob",
            score_gradient,
            shared_key_heads,
            preferred_element_type=single_precision,
        )
        * score_scale
    )
    query_gradient_piece = query_gradient_piece.reshape(rows, -1)
    key_gradient_piece = (
        jnp.einsum(
            "nkjv,jnka->vna", score_gradient, query_tensor4, preferred_element_type=single_precision
        )
        * score_scale
    )
    value_gradient_piece = jnp.einsum(
        "nkjv,jnka->vna", probabilities16, output_gradient4, preferred_element_type=single_precision
    )
    own_keys, own_values = (
        lax.psum_scatter(
            key_gradient_piece.reshape(span, -1).astype(jnp.bfloat16),
            "sp",
            scatter_dimension=0,
            tiled=True,
        ).astype(jnp.float32),
        lax.psum_scatter(
            value_gradient_piece.reshape(span, -1).astype(jnp.bfloat16),
            "sp",
            scatter_dimension=0,
            tiled=True,
        ).astype(jnp.float32),
    )
    stacked = jnp.concatenate(
        [own_keys.astype(jnp.bfloat16), own_values.astype(jnp.bfloat16)], axis=1
    )
    group = lax.all_gather(stacked, "tp", axis=0, tiled=True)
    weights = jnp.concatenate([w_key, w_value], axis=1)
    d_source = lax.dot_general(
        group, weights, (((1,), (1,)), ((), ())), preferred_element_type=single_precision
    ).astype(jnp.bfloat16)
    kv_width = w_value.shape[1]
    weight_term = lax.dot_general(
        source,
        group[:, kv_width:],
        (((0,), (0,)), ((), ())),
        preferred_element_type=single_precision,
    )
    d_wvalue = lax.psum(weight_term.astype(jnp.bfloat16), "sp").astype(jnp.float32)
    dq16 = lax.psum(query_gradient_piece, "tp").astype(jnp.bfloat16)
    d_target = lax.dot_general(
        dq16, w_query, (((1,), (1,)), ((), ())), preferred_element_type=single_precision
    ).astype(jnp.bfloat16)
    return (d_target, d_source, d_wvalue)


def solution(mesh):
    body = functools.partial(shards, mesh.shape["sp"], mesh.shape["tp"])
    in_specs = (
        P("sp", None),
        P("sp", None),
        P("sp", None),
        P("sp", None),
        P(("sp", "tp"), None),
        P(("sp", "tp"), None),
        P("sp", "tp"),
        P("tp", None),
        P("tp", None),
        P("tp", None),
    )
    out_specs = (P("sp", "tp"), P("sp", "tp"), P("tp", None))
    return jax.shard_map(body, mesh=mesh, in_specs=in_specs, out_specs=out_specs, check_vma=False)
```

```python
import functools
import math

import jax
import jax.numpy as jnp
from jax import lax
from jax.experimental import pallas as pl
from jax.experimental.pallas import tpu as pltpu
from jax.sharding import PartitionSpec as P

HEADS = 12
KV_HEADS = 2
HEAD_DIM = 256
CORES = 2
SIDE = 2
VMEM_BYTES = 60 * 1024 * 1024
MESH = pl.DeviceIdType.MESH
NT = (((1,), (1,)), ((), ()))
TN = (((0,), (0,)), ((), ()))
F32 = jnp.float32
BF16 = jnp.bfloat16


def dot(a, b, dims=(((1,), (0,)), ((), ()))):
    return lax.dot_general(a, b, dims, preferred_element_type=F32)


def kernel(
    sp, tp, lse_ref, k_ref, v_ref, q_hbm, o_hbm, do_hbm, src_hbm, wq_hbm, wk_hbm, wv_hbm,
    dt_hbm, ds_hbm, dw_hbm,
    dt_ref, ds_ref, dw_ref, kv, qs, dos, os_, wq, wk, wv, src, src_t, lse, delta, dqa, dq16, part, got, full,
    load_sem, near_send, near_recv, kv_send, kv_recv, kv_pair_send, kv_pair_recv,
    src_send, src_recv, part_send, part_recv, g_send, g_recv, gy_send, gy_recv, gp_send, gp_recv, kvz_send, gz_send,
):
    rows = q_hbm.shape[0]
    rs, kw = k_ref.shape
    repeat = HEADS // KV_HEADS
    scale = 1.0 / math.sqrt(HEAD_DIM)
    i, j = lax.axis_index("sp"), lax.axis_index("tp")
    ny, nz = sp // CORES, tp // SIDE
    y, c = i // CORES, lax.rem(i, CORES)
    z, x = j // SIDE, lax.rem(j, SIDE)
    sp_peers = [lax.rem(i + k, sp) for k in range(1, sp)]
    y_peers = [lax.rem(y + k, ny) * CORES + c for k in range(1, ny)]
    pair = y * CORES + 1 - c
    orders = [sorted((b for b in range(nz) if b != a), key=lambda b, a=a: abs(a - b)) for a in range(nz)]
    zs = [sum(jnp.where(z == a, order[n], 0) for a, order in enumerate(orders)) for n in range(nz - 1)]
    onward = [jnp.where(a > z, z - 1, z + 1) for a in zs]
    onward_ok = [(b >= 0) & (b < nz) for b in onward]
    z_peers = [a * SIDE + x for a in zs]
    jx = z * SIDE + 1 - x
    sends = []
    maybe_sends = []

    def send_if(condition, make):
        pl.when(condition)(lambda: make().start())
        maybe_sends.append((condition, make))

    def along_z(ref, n, s, r):
        targets = [(z + 1, z + 1 < nz, 0), (z - 1, z >= 1, 1)] if n is None else [(onward[n], onward_ok[n], n + 2)]
        for to, ok, at in targets:
            send_if(ok, lambda to=to, at=at: pltpu.make_async_remote_copy(
                src_ref=ref, dst_ref=ref, send_sem=s.at[at], recv_sem=r,
                device_id=(i, to * SIDE + x), device_id_type=MESH,
            ))

    def send(ref_from, ref_to, s, r, device):
        copy = pltpu.make_async_remote_copy(
            src_ref=ref_from, dst_ref=ref_to, send_sem=s, recv_sem=r,
            device_id=device, device_id_type=MESH,
        )
        copy.start()
        sends.append(copy)

    def receive(ref, r):
        pltpu.make_async_remote_copy(
            src_ref=ref, dst_ref=ref, send_sem=load_sem.at[0], recv_sem=r,
            device_id=(pair, j), device_id_type=MESH,
        ).wait_recv()

    loads = []

    def load(ref_from, ref_to):
        copy = pltpu.make_async_copy(ref_from, ref_to, load_sem.at[len(loads)])
        copy.start()
        loads.append(copy)
        return copy

    barrier = pltpu.get_barrier_semaphore()
    near = [(p, j) for p in sp_peers] + [(i, p) for p in z_peers] + [(i, jx)]
    for d in near:
        pl.semaphore_signal(barrier, inc=1, device_id=d, device_id_type=MESH)
    near_rows = pl.ds(pl.multiple_of(i * rs, rs), rs)
    own_copies = [load(r, kv.at[t, j, near_rows]) for t, r in enumerate((k_ref, v_ref))]
    attn_loads = []
    for g in range(KV_HEADS):
        for h in range(repeat):
            columns = pl.ds((g * repeat + h) * HEAD_DIM, HEAD_DIM)
            for a, b in ((q_hbm, qs), (do_hbm, dos), (o_hbm, os_)):
                attn_loads.append(load(a.at[:, columns], b.at[g, pl.ds(h * rows, rows)]))
    src_load = load(src_hbm, src.at[i])
    weight_loads = [load(wq_hbm, wq), load(wk_hbm, wk), load(wv_hbm, wv)]
    pl.semaphore_wait(barrier, len(near))

    for n, p in enumerate(sp_peers):
        for t, r in enumerate((k_ref, v_ref)):
            send(r, kv.at[t, j, near_rows], near_send.at[t, n], near_recv.at[t, i], (p, j))

    for copy in attn_loads:
        copy.wait()
    for g in range(KV_HEADS):
        for h in range(repeat):
            at = pl.ds(h * rows, rows)
            d = jnp.sum(dos[g, at].astype(F32) * os_[g, at].astype(F32), axis=1, keepdims=True)
            delta[g, at] = jnp.broadcast_to(d, (rows, 128))
            n = g * repeat + h
            lse[g, at] = jnp.transpose(jnp.broadcast_to(lse_ref[n:n + 1, :], (128, rows)))

    for copy in own_copies:
        copy.wait()
    for p in sp_peers:
        for t in range(2):
            receive(kv.at[t, j, pl.ds(pl.multiple_of(p * rs, rs), rs)], near_recv.at[t, p])

    def kv_to_x(slot, n):
        send(kv.at[c, slot], kv.at[c, slot], kv_send.at[n], kv_recv.at[slot], (i, jx))

    def kv_to_pair(slot):
        send(kv.at[c, slot], kv.at[c, slot], kv_pair_send.at[slot], kv_pair_recv.at[slot], (pair, j))

    kv_to_x(j, 0)
    along_z(kv.at[c, j], None, kvz_send, kv_recv.at[j])

    def wide(a, n):
        return a if n == 1 else jnp.concatenate([a] * n, axis=1)

    def grads(g, keys, values):
        n = keys.shape[0] // 128
        p = jnp.exp(dot(qs[g], keys, NT) * scale - wide(lse[g], n))
        dp = dot(dos[g], values, NT)
        ds = (p * (dp - wide(delta[g], n))).astype(BF16)
        return p, ds

    def head_columns(g):
        return slice(g * HEAD_DIM, (g + 1) * HEAD_DIM)

    for g in range(KV_HEADS):
        cols = head_columns(g)
        keys = kv[0, j, :, cols]
        p, ds = grads(g, keys, kv[1, j, :, cols])
        dk = dot(ds, qs[g], TN) * scale
        dv = dot(p.astype(BF16), dos[g], TN)
        part[:, 0, :, cols] = dk.astype(BF16).reshape(sp, rs, HEAD_DIM)
        part[:, 1, :, cols] = dv.astype(BF16).reshape(sp, rs, HEAD_DIM)
        dqa[g] = dot(ds, keys)
    for n, p in enumerate(sp_peers):
        send(part.at[p], got.at[i], part_send.at[n], part_recv.at[i], (p, j))
    src_load.wait()
    for n, p in enumerate(y_peers):
        send(src.at[i], src.at[i], src_send.at[n], src_recv.at[i], (p, j))
    send(src.at[i], src.at[i], src_send.at[ny], src_recv.at[i], (pair, j))

    def chunk_one(slot):
        for g in range(KV_HEADS):
            cols = head_columns(g)
            keys = kv[0, slot, :, cols]
            _, ds = grads(g, keys, kv[1, slot, :, cols])
            dqa[g] += dot(ds, keys)

    def chunk_z(a):
        slots = pl.ds(a * SIDE, SIDE)
        for g in range(KV_HEADS):
            cols = head_columns(g)
            keys = kv[0, slots, :, cols].reshape(-1, HEAD_DIM)
            values = kv[1, slots, :, cols].reshape(-1, HEAD_DIM)
            _, ds = grads(g, keys, values)
            dqa[g] += dot(ds, keys)

    def from_z(n):
        slot = z_peers[n]
        receive(kv.at[c, slot], kv_recv.at[slot])
        along_z(kv.at[c, slot], n, kvz_send, kv_recv.at[slot])
        kv_to_x(slot, n + 1)
        kv_to_pair(slot)

    def from_x(slot):
        receive(kv.at[c, slot], kv_recv.at[slot])
        kv_to_pair(slot)

    def from_pair(slot):
        receive(kv.at[1 - c, slot], kv_pair_recv.at[slot])

    def g_to_x(slot, n):
        send(full.at[i, slot], full.at[i, slot], g_send.at[n], g_recv.at[slot], (i, jx))

    def g_spread(slot):
        for n, p in enumerate(y_peers):
            send(full.at[i, slot, 1], full.at[i, slot, 1], gy_send.at[n, slot], gy_recv.at[i, slot], (p, j))
        send(full.at[i, slot, 1], full.at[i, slot, 1], gp_send.at[i, slot], gp_recv.at[i, slot], (pair, j))

    def g_from_z(n):
        slot = z_peers[n]
        receive(full.at[i, slot], g_recv.at[slot])
        along_z(full.at[i, slot], n, gz_send, g_recv.at[slot])
        g_to_x(slot, n + 1)
        g_spread(slot)

    def g_from_x(slot):
        receive(full.at[i, slot], g_recv.at[slot])
        g_spread(slot)

    def g_from_y(slot):
        for p in y_peers:
            receive(full.at[p, slot, 1], gy_recv.at[p, slot])
            send(full.at[p, slot, 1], full.at[p, slot, 1], gp_send.at[p, slot], gp_recv.at[p, slot], (pair, j))

    far = [a * SIDE + 1 - x for a in zs]
    from_x(jx)
    from_z(0)
    total = part[i].astype(F32)
    for p in sp_peers:
        receive(got.at[p], part_recv.at[p])
        total += got[p].astype(F32)
    full[i, j] = total.astype(BF16)
    along_z(full.at[i, j], None, gz_send, g_recv.at[j])
    g_to_x(j, 0)
    g_spread(j)
    from_pair(jx)
    chunk_one(jx)
    for n in range(nz - 1):
        if n + 1 < nz - 1:
            from_z(n + 1)
        from_x(far[n])
        g_from_z(n)
        if n == 0:
            g_from_x(jx)
            for m, p in enumerate(y_peers):
                receive(src.at[p], src_recv.at[p])
                send(src.at[p], src.at[p], src_send.at[ny + 1 + m], src_recv.at[p], (pair, j))
        else:
            g_from_x(far[n - 1])
        g_from_y([j, jx, z_peers[0]][n])
        from_pair(z_peers[n])
        from_pair(far[n])
        chunk_z(zs[n])
    g_from_x(far[nz - 2])
    for copy in weight_loads:
        copy.wait()
    for g in range(KV_HEADS):
        for h in range(repeat):
            n = g * repeat + h
            dq16[:, n * HEAD_DIM:(n + 1) * HEAD_DIM] = (dqa[g, h * rows:(h + 1) * rows] * scale).astype(BF16)
    theirs = [lax.rem(y + k, ny) * CORES + 1 - c for k in range(ny)]
    for p in theirs:
        receive(src.at[p], src_recv.at[p])
    for b in range(sp):
        src_t[b] = jnp.transpose(src[b])
    dt_ref[...] = dot(dq16[...], wq[...], NT).astype(BF16)
    results = [load(dt_ref, dt_hbm)]
    for slot in z_peers[1:] + far:
        g_from_y(slot)
    ds_ref[...] = (
        dot(full[i, :, 0].reshape(-1, kw), wk[...], NT) + dot(full[i, :, 1].reshape(-1, kw), wv[...], NT)
    ).astype(BF16)
    results.append(load(ds_ref, ds_hbm))
    for p in theirs:
        for slot in range(tp):
            receive(full.at[p, slot, 1], gp_recv.at[p, slot])
    dw = dot(src_t[0], full[0, :, 1].reshape(-1, kw))
    for b in range(1, sp):
        dw += dot(src_t[b], full[b, :, 1].reshape(-1, kw))
    dw_ref[...] = dw
    results.append(load(dw_ref, dw_hbm))
    for copy in results:
        copy.wait()
    for copy in sends:
        copy.wait_send()
    for condition, make in maybe_sends:
        pl.when(condition)(lambda make=make: make().wait_send())


def settle(*refs):
    count = (len(refs) - 1) // 3
    sems = refs[-1]
    ins, outs, held = (refs[n * count:(n + 1) * count] for n in range(3))
    steps = []
    for n in range(count):
        tall = ins[n].shape[0]
        pieces = 4 if n == count - 1 and tall % 32 == 0 else 1
        for m in range(pieces):
            at = pl.ds(m * (tall // pieces), tall // pieces)
            k = len(steps)
            steps.append((
                pltpu.make_async_copy(ins[n].at[at], held[n].at[at], sems.at[0, k]),
                pltpu.make_async_copy(held[n].at[at], outs[n].at[at], sems.at[1, k]),
            ))
    for arrive, _ in steps:
        arrive.start()
    for arrive, leave in steps:
        arrive.wait()
        leave.start()
    for _, leave in steps:
        leave.wait()


def settled(arrays):
    hbm = pl.BlockSpec(memory_space=pl.ANY)
    return pl.pallas_call(
        settle,
        out_shape=tuple(jax.ShapeDtypeStruct(a.shape, a.dtype) for a in arrays),
        in_specs=[hbm] * len(arrays),
        out_specs=(hbm,) * len(arrays),
        scratch_shapes=[pltpu.VMEM(a.shape, a.dtype) for a in arrays] + [
            pltpu.SemaphoreType.DMA((2, len(arrays) + 3))
        ],
        compiler_params=pltpu.CompilerParams(vmem_limit_bytes=VMEM_BYTES),
    )(*arrays)


def fused(sp, tp, scratch, queries, attn_out, log_norm, cotangent, keys, values, source, w_query, w_key, w_value):
    rows = queries.shape[0]
    width = w_value.shape[0]
    vmem, hbm = pl.BlockSpec(memory_space=pltpu.VMEM), pl.BlockSpec(memory_space=pl.ANY)
    dma = pltpu.SemaphoreType.DMA
    nz, ny = tp // SIDE, sp // CORES
    return settled(pl.pallas_call(
        functools.partial(kernel, sp, tp),
        out_shape=(
            jax.ShapeDtypeStruct((rows, width), BF16),
            jax.ShapeDtypeStruct((source.shape[0], width), BF16),
            jax.ShapeDtypeStruct(w_value.shape, F32),
        ),
        in_specs=[vmem] * 3 + [hbm] * 7,
        out_specs=(hbm,) * 3,
        scratch_shapes=[
            pltpu.VMEM((rows, width), BF16), pltpu.VMEM((source.shape[0], width), BF16), pltpu.VMEM(w_value.shape, F32),
        ] + [pltpu.VMEM(s, t) for s, t in scratch] + [
            dma((3 * HEADS + 9,)), dma((2, sp)), dma((2, sp)), dma((2 * nz,)), dma((tp,)), dma((tp,)), dma((tp,)),
            dma((2 * ny,)), dma((sp,)), dma((sp,)), dma((sp,)), dma((2 * nz,)), dma((tp,)),
            dma((ny, tp)), dma((sp, tp)), dma((sp, tp)), dma((sp, tp)), dma((nz + 1,)), dma((nz + 1,)),
        ],
        compiler_params=pltpu.CompilerParams(
            collective_id=0, has_side_effects=True, vmem_limit_bytes=VMEM_BYTES
        ),
    )(log_norm.T, keys, values, queries, attn_out, cotangent, source, w_query, w_key, w_value))


def scratch_of(sp, tp, queries, keys, source, w_query, w_value):
    rows, width = queries.shape
    rs, kw = keys.shape
    stack = (KV_HEADS, rows * HEADS // KV_HEADS, HEAD_DIM)
    flat = stack[:2] + (128,)
    return [
        ((2, tp, sp * rs, kw), BF16), (stack, BF16), (stack, BF16), (stack, BF16),
        (w_query.shape, BF16), (w_value.shape, BF16), (w_value.shape, BF16),
        ((sp,) + source.shape, BF16), ((sp,) + source.shape[::-1], BF16), (flat, F32), (flat, F32), (stack, F32), ((rows, width), BF16),
        ((sp, 2, rs, kw), BF16), ((sp, 2, rs, kw), BF16), ((sp, tp, 2, rs, kw), BF16),
    ]


def shards(sp, tp, *args):
    queries, _, _, _, keys, _, source, w_query, _, w_value = args
    scratch = scratch_of(sp, tp, queries, keys, source, w_query, w_value)
    size = sum(math.prod(s) * jnp.dtype(t).itemsize for s, t in scratch)
    fits = size * 2 < VMEM_BYTES and sp * keys.shape[0] == 128
    if fits and sp % CORES == 0 and tp == 4 * SIDE:
        return fused(sp, tp, scratch, *args)
    return plain(*args)


def plain(queries, attn_out, log_norm, cotangent, keys, values, source, w_query, w_key, w_value):
    single_precision = jnp.float32
    repeat = HEADS // KV_HEADS
    score_scale = 1.0 / math.sqrt(HEAD_DIM)
    rows = queries.shape[0]
    near_keys, near_values = (
        lax.all_gather(keys, "sp", axis=0, tiled=True),
        lax.all_gather(values, "sp", axis=0, tiled=True),
    )
    span = near_keys.shape[0]
    query_tensor4 = queries.reshape(rows, KV_HEADS, repeat, HEAD_DIM)
    output_gradient4 = cotangent.reshape(rows, KV_HEADS, repeat, HEAD_DIM)
    out4 = attn_out.reshape(rows, KV_HEADS, repeat, HEAD_DIM)
    shared_key_heads = near_keys.reshape(span, KV_HEADS, HEAD_DIM)
    shared_value_heads = near_values.reshape(span, KV_HEADS, HEAD_DIM)
    delta = jnp.sum(
        output_gradient4.astype(single_precision) * out4.astype(single_precision), axis=3
    )
    delta = jnp.transpose(delta, (1, 2, 0))[..., None]
    lse = jnp.transpose(log_norm.reshape(rows, KV_HEADS, repeat), (1, 2, 0))[..., None]
    logit_scores = (
        jnp.einsum(
            "znjk,wnk->njzw",
            query_tensor4,
            shared_key_heads,
            preferred_element_type=single_precision,
        )
        * score_scale
    )
    probs = jnp.exp(logit_scores - lse)
    probabilities16 = probs.astype(jnp.bfloat16)
    prob_gradient = jnp.einsum(
        "znjk,wnk->njzw",
        output_gradient4,
        shared_value_heads,
        preferred_element_type=single_precision,
    )
    score_gradient = (probs * (prob_gradient - delta)).astype(jnp.bfloat16)
    query_gradient_piece = (
        jnp.einsum(
            "wohn,nwb->hwob",
            score_gradient,
            shared_key_heads,
            preferred_element_type=single_precision,
        )
        * score_scale
    )
    query_gradient_piece = query_gradient_piece.reshape(rows, -1)
    key_gradient_piece = (
        jnp.einsum(
            "nkjv,jnka->vna", score_gradient, query_tensor4, preferred_element_type=single_precision
        )
        * score_scale
    )
    value_gradient_piece = jnp.einsum(
        "nkjv,jnka->vna", probabilities16, output_gradient4, preferred_element_type=single_precision
    )
    own_keys, own_values = (
        lax.psum_scatter(
            key_gradient_piece.reshape(span, -1).astype(jnp.bfloat16),
            "sp",
            scatter_dimension=0,
            tiled=True,
        ).astype(jnp.float32),
        lax.psum_scatter(
            value_gradient_piece.reshape(span, -1).astype(jnp.bfloat16),
            "sp",
            scatter_dimension=0,
            tiled=True,
        ).astype(jnp.float32),
    )
    stacked = jnp.concatenate(
        [own_keys.astype(jnp.bfloat16), own_values.astype(jnp.bfloat16)], axis=1
    )
    group = lax.all_gather(stacked, "tp", axis=0, tiled=True)
    weights = jnp.concatenate([w_key, w_value], axis=1)
    d_source = lax.dot_general(
        group, weights, (((1,), (1,)), ((), ())), preferred_element_type=single_precision
    ).astype(jnp.bfloat16)
    kv_width = w_value.shape[1]
    weight_term = lax.dot_general(
        source,
        group[:, kv_width:],
        (((0,), (0,)), ((), ())),
        preferred_element_type=single_precision,
    )
    d_wvalue = lax.psum(weight_term.astype(jnp.bfloat16), "sp").astype(jnp.float32)
    dq16 = lax.psum(query_gradient_piece, "tp").astype(jnp.bfloat16)
    d_target = lax.dot_general(
        dq16, w_query, (((1,), (1,)), ((), ())), preferred_element_type=single_precision
    ).astype(jnp.bfloat16)
    return (d_target, d_source, d_wvalue)


def solution(mesh):
    body = functools.partial(shards, mesh.shape["sp"], mesh.shape["tp"])
    in_specs = (
        P("sp", None),
        P("sp", None),
        P("sp", None),
        P("sp", None),
        P(("sp", "tp"), None),
        P(("sp", "tp"), None),
        P("sp", "tp"),
        P("tp", None),
        P("tp", None),
        P("tp", None),
    )
    out_specs = (P("sp", "tp"), P("sp", "tp"), P("tp", None))
    return jax.shard_map(body, mesh=mesh, in_specs=in_specs, out_specs=out_specs, check_vma=False)
```

```python
import functools
import math

import jax
import jax.numpy as jnp
from jax import lax
from jax.experimental import pallas as pl
from jax.experimental.pallas import tpu as pltpu
from jax.sharding import PartitionSpec as P

HEADS = 12
KV_HEADS = 2
HEAD_DIM = 256
CORES = 2
SIDE = 2
VMEM_BYTES = 60 * 1024 * 1024
MESH = pl.DeviceIdType.MESH
NT = (((1,), (1,)), ((), ()))
TN = (((0,), (0,)), ((), ()))
F32 = jnp.float32
BF16 = jnp.bfloat16


def dot(a, b, dims=(((1,), (0,)), ((), ()))):
    return lax.dot_general(a, b, dims, preferred_element_type=F32)


def kernel(
    sp, tp, lse_ref, k_ref, v_ref, q_hbm, o_hbm, do_hbm, src_hbm, wq_hbm, wk_hbm, wv_hbm,
    dt_hbm, ds_hbm, dw_hbm,
    dt_ref, ds_ref, dw_ref, kv, qs, dos, os_, wq, wk, wv, src, src_t, lse, delta, dqa, dq16, part, got, full,
    load_sem, near_send, near_recv, kv_send, kv_recv, kv_pair_send, kv_pair_recv,
    src_send, src_recv, part_send, part_recv, g_send, g_recv, gy_send, gy_recv, gp_send, gp_recv, kvz_send, gz_send,
):
    rows = q_hbm.shape[0]
    rs, kw = k_ref.shape
    repeat = HEADS // KV_HEADS
    scale = 1.0 / math.sqrt(HEAD_DIM)
    i, j = lax.axis_index("sp"), lax.axis_index("tp")
    ny, nz = sp // CORES, tp // SIDE
    y, c = i // CORES, lax.rem(i, CORES)
    z, x = j // SIDE, lax.rem(j, SIDE)
    sp_peers = [lax.rem(i + k, sp) for k in range(1, sp)]
    y_peers = [lax.rem(y + k, ny) * CORES + c for k in range(1, ny)]
    pair = y * CORES + 1 - c
    orders = [sorted((b for b in range(nz) if b != a), key=lambda b, a=a: abs(a - b)) for a in range(nz)]
    zs = [sum(jnp.where(z == a, order[n], 0) for a, order in enumerate(orders)) for n in range(nz - 1)]
    onward = [jnp.where(a > z, z - 1, z + 1) for a in zs]
    onward_ok = [(b >= 0) & (b < nz) for b in onward]
    z_peers = [a * SIDE + x for a in zs]
    jx = z * SIDE + 1 - x
    sends = []
    maybe_sends = []

    def send_if(condition, make):
        pl.when(condition)(lambda: make().start())
        maybe_sends.append((condition, make))

    def along_z(ref, n, s, r):
        targets = [(z + 1, z + 1 < nz, 0), (z - 1, z >= 1, 1)] if n is None else [(onward[n], onward_ok[n], n + 2)]
        for to, ok, at in targets:
            send_if(ok, lambda to=to, at=at: pltpu.make_async_remote_copy(
                src_ref=ref, dst_ref=ref, send_sem=s.at[at], recv_sem=r,
                device_id=(i, to * SIDE + x), device_id_type=MESH,
            ))

    def send(ref_from, ref_to, s, r, device):
        copy = pltpu.make_async_remote_copy(
            src_ref=ref_from, dst_ref=ref_to, send_sem=s, recv_sem=r,
            device_id=device, device_id_type=MESH,
        )
        copy.start()
        sends.append(copy)

    def receive(ref, r):
        pltpu.make_async_remote_copy(
            src_ref=ref, dst_ref=ref, send_sem=load_sem.at[0], recv_sem=r,
            device_id=(pair, j), device_id_type=MESH,
        ).wait_recv()

    loads = []

    def load(ref_from, ref_to):
        copy = pltpu.make_async_copy(ref_from, ref_to, load_sem.at[len(loads)])
        copy.start()
        loads.append(copy)
        return copy

    barrier = pltpu.get_barrier_semaphore()
    near = [(p, j) for p in sp_peers] + [(i, p) for p in z_peers] + [(i, jx)]
    for d in near:
        pl.semaphore_signal(barrier, inc=1, device_id=d, device_id_type=MESH)
    near_rows = pl.ds(pl.multiple_of(i * rs, rs), rs)
    own_copies = [load(r, kv.at[t, j, near_rows]) for t, r in enumerate((k_ref, v_ref))]
    attn_loads = []
    for g in range(KV_HEADS):
        for h in range(repeat):
            columns = pl.ds((g * repeat + h) * HEAD_DIM, HEAD_DIM)
            for a, b in ((q_hbm, qs), (do_hbm, dos), (o_hbm, os_)):
                attn_loads.append(load(a.at[:, columns], b.at[g, pl.ds(h * rows, rows)]))
    src_load = load(src_hbm, src.at[i])
    weight_loads = [load(wq_hbm, wq), load(wk_hbm, wk), load(wv_hbm, wv)]
    pl.semaphore_wait(barrier, len(near))

    for n, p in enumerate(sp_peers):
        for t, r in enumerate((k_ref, v_ref)):
            send(r, kv.at[t, j, near_rows], near_send.at[t, n], near_recv.at[t, i], (p, j))

    for copy in attn_loads:
        copy.wait()
    for g in range(KV_HEADS):
        for h in range(repeat):
            at = pl.ds(h * rows, rows)
            d = jnp.sum(dos[g, at].astype(F32) * os_[g, at].astype(F32), axis=1, keepdims=True)
            delta[g, at] = jnp.broadcast_to(d, (rows, 128))
            n = g * repeat + h
            lse[g, at] = jnp.transpose(jnp.broadcast_to(lse_ref[n:n + 1, :], (128, rows)))

    for copy in own_copies:
        copy.wait()
    for p in sp_peers:
        for t in range(2):
            receive(kv.at[t, j, pl.ds(pl.multiple_of(p * rs, rs), rs)], near_recv.at[t, p])

    def kv_to_x(slot, n):
        send(kv.at[c, slot], kv.at[c, slot], kv_send.at[n], kv_recv.at[slot], (i, jx))

    def kv_to_pair(slot):
        send(kv.at[c, slot], kv.at[c, slot], kv_pair_send.at[slot], kv_pair_recv.at[slot], (pair, j))

    kv_to_x(j, 0)
    along_z(kv.at[c, j], None, kvz_send, kv_recv.at[j])

    def wide(a, n):
        return a if n == 1 else jnp.concatenate([a] * n, axis=1)

    def grads(g, keys, values):
        n = keys.shape[0] // 128
        p = jnp.exp(dot(qs[g], keys, NT) * scale - wide(lse[g], n))
        dp = dot(dos[g], values, NT)
        ds = (p * (dp - wide(delta[g], n))).astype(BF16)
        return p, ds

    def head_columns(g):
        return slice(g * HEAD_DIM, (g + 1) * HEAD_DIM)

    for g in range(KV_HEADS):
        cols = head_columns(g)
        keys = kv[0, j, :, cols]
        p, ds = grads(g, keys, kv[1, j, :, cols])
        dk = dot(ds, qs[g], TN) * scale
        dv = dot(p.astype(BF16), dos[g], TN)
        part[:, 0, :, cols] = dk.astype(BF16).reshape(sp, rs, HEAD_DIM)
        part[:, 1, :, cols] = dv.astype(BF16).reshape(sp, rs, HEAD_DIM)
        dqa[g] = dot(ds, keys)
    for n, p in enumerate(sp_peers):
        send(part.at[p], got.at[i], part_send.at[n], part_recv.at[i], (p, j))

    def chunk_one(slot):
        for g in range(KV_HEADS):
            cols = head_columns(g)
            keys = kv[0, slot, :, cols]
            _, ds = grads(g, keys, kv[1, slot, :, cols])
            dqa[g] += dot(ds, keys)

    def chunk_z(a):
        slots = pl.ds(a * SIDE, SIDE)
        for g in range(KV_HEADS):
            cols = head_columns(g)
            keys = kv[0, slots, :, cols].reshape(-1, HEAD_DIM)
            values = kv[1, slots, :, cols].reshape(-1, HEAD_DIM)
            _, ds = grads(g, keys, values)
            dqa[g] += dot(ds, keys)

    def from_z(n):
        slot = z_peers[n]
        receive(kv.at[c, slot], kv_recv.at[slot])
        along_z(kv.at[c, slot], n, kvz_send, kv_recv.at[slot])
        kv_to_x(slot, n + 1)
        kv_to_pair(slot)

    def from_x(slot):
        receive(kv.at[c, slot], kv_recv.at[slot])
        kv_to_pair(slot)

    def from_pair(slot):
        receive(kv.at[1 - c, slot], kv_pair_recv.at[slot])

    def g_to_x(slot, n):
        send(full.at[i, slot], full.at[i, slot], g_send.at[n], g_recv.at[slot], (i, jx))

    def g_spread(slot):
        for n, p in enumerate(y_peers):
            send(full.at[i, slot, 1], full.at[i, slot, 1], gy_send.at[n, slot], gy_recv.at[i, slot], (p, j))
        send(full.at[i, slot, 1], full.at[i, slot, 1], gp_send.at[i, slot], gp_recv.at[i, slot], (pair, j))

    def g_from_z(n):
        slot = z_peers[n]
        receive(full.at[i, slot], g_recv.at[slot])
        along_z(full.at[i, slot], n, gz_send, g_recv.at[slot])
        g_to_x(slot, n + 1)
        g_spread(slot)

    def g_from_x(slot):
        receive(full.at[i, slot], g_recv.at[slot])
        g_spread(slot)

    def g_from_y(slot):
        for p in y_peers:
            receive(full.at[p, slot, 1], gy_recv.at[p, slot])
            send(full.at[p, slot, 1], full.at[p, slot, 1], gp_send.at[p, slot], gp_recv.at[p, slot], (pair, j))

    far = [a * SIDE + 1 - x for a in zs]
    from_x(jx)
    from_z(0)
    total = part[i].astype(F32)
    for p in sp_peers:
        receive(got.at[p], part_recv.at[p])
        total += got[p].astype(F32)
    full[i, j] = total.astype(BF16)
    along_z(full.at[i, j], None, gz_send, g_recv.at[j])
    g_to_x(j, 0)
    g_spread(j)
    src_load.wait()
    for n, p in enumerate(y_peers):
        send(src.at[i], src.at[i], src_send.at[n], src_recv.at[i], (p, j))
    send(src.at[i], src.at[i], src_send.at[ny], src_recv.at[i], (pair, j))
    from_pair(jx)
    chunk_one(jx)
    for n in range(nz - 1):
        if n + 1 < nz - 1:
            from_z(n + 1)
        from_x(far[n])
        g_from_z(n)
        if n == 0:
            g_from_x(jx)
        else:
            g_from_x(far[n - 1])
        if n == 1:
            for m, p in enumerate(y_peers):
                receive(src.at[p], src_recv.at[p])
                send(src.at[p], src.at[p], src_send.at[ny + 1 + m], src_recv.at[p], (pair, j))
        g_from_y([j, jx, z_peers[0]][n])
        from_pair(z_peers[n])
        from_pair(far[n])
        chunk_z(zs[n])
    g_from_x(far[nz - 2])
    for copy in weight_loads:
        copy.wait()
    for g in range(KV_HEADS):
        for h in range(repeat):
            n = g * repeat + h
            dq16[:, n * HEAD_DIM:(n + 1) * HEAD_DIM] = (dqa[g, h * rows:(h + 1) * rows] * scale).astype(BF16)
    theirs = [lax.rem(y + k, ny) * CORES + 1 - c for k in range(ny)]
    for p in theirs:
        receive(src.at[p], src_recv.at[p])
    for b in range(sp):
        src_t[b] = jnp.transpose(src[b])
    dt_ref[...] = dot(dq16[...], wq[...], NT).astype(BF16)
    results = [load(dt_ref, dt_hbm)]
    for slot in z_peers[1:] + far:
        g_from_y(slot)
    ds_ref[...] = (
        dot(full[i, :, 0].reshape(-1, kw), wk[...], NT) + dot(full[i, :, 1].reshape(-1, kw), wv[...], NT)
    ).astype(BF16)
    results.append(load(ds_ref, ds_hbm))
    for p in theirs:
        for slot in range(tp):
            receive(full.at[p, slot, 1], gp_recv.at[p, slot])
    dw = dot(src_t[0], full[0, :, 1].reshape(-1, kw))
    for b in range(1, sp):
        dw += dot(src_t[b], full[b, :, 1].reshape(-1, kw))
    dw_ref[...] = dw
    results.append(load(dw_ref, dw_hbm))
    for copy in results:
        copy.wait()
    for copy in sends:
        copy.wait_send()
    for condition, make in maybe_sends:
        pl.when(condition)(lambda make=make: make().wait_send())


def settle(*refs):
    count = (len(refs) - 1) // 3
    sems = refs[-1]
    ins, outs, held = (refs[n * count:(n + 1) * count] for n in range(3))
    steps = []
    for n in range(count):
        tall = ins[n].shape[0]
        pieces = 4 if n == count - 1 and tall % 32 == 0 else 1
        for m in range(pieces):
            at = pl.ds(m * (tall // pieces), tall // pieces)
            k = len(steps)
            steps.append((
                pltpu.make_async_copy(ins[n].at[at], held[n].at[at], sems.at[0, k]),
                pltpu.make_async_copy(held[n].at[at], outs[n].at[at], sems.at[1, k]),
            ))
    for arrive, _ in steps:
        arrive.start()
    for arrive, leave in steps:
        arrive.wait()
        leave.start()
    for _, leave in steps:
        leave.wait()


def settled(arrays):
    hbm = pl.BlockSpec(memory_space=pl.ANY)
    return pl.pallas_call(
        settle,
        out_shape=tuple(jax.ShapeDtypeStruct(a.shape, a.dtype) for a in arrays),
        in_specs=[hbm] * len(arrays),
        out_specs=(hbm,) * len(arrays),
        scratch_shapes=[pltpu.VMEM(a.shape, a.dtype) for a in arrays] + [
            pltpu.SemaphoreType.DMA((2, len(arrays) + 3))
        ],
        compiler_params=pltpu.CompilerParams(vmem_limit_bytes=VMEM_BYTES),
    )(*arrays)


def fused(sp, tp, scratch, queries, attn_out, log_norm, cotangent, keys, values, source, w_query, w_key, w_value):
    rows = queries.shape[0]
    width = w_value.shape[0]
    vmem, hbm = pl.BlockSpec(memory_space=pltpu.VMEM), pl.BlockSpec(memory_space=pl.ANY)
    dma = pltpu.SemaphoreType.DMA
    nz, ny = tp // SIDE, sp // CORES
    return settled(pl.pallas_call(
        functools.partial(kernel, sp, tp),
        out_shape=(
            jax.ShapeDtypeStruct((rows, width), BF16),
            jax.ShapeDtypeStruct((source.shape[0], width), BF16),
            jax.ShapeDtypeStruct(w_value.shape, F32),
        ),
        in_specs=[vmem] * 3 + [hbm] * 7,
        out_specs=(hbm,) * 3,
        scratch_shapes=[
            pltpu.VMEM((rows, width), BF16), pltpu.VMEM((source.shape[0], width), BF16), pltpu.VMEM(w_value.shape, F32),
        ] + [pltpu.VMEM(s, t) for s, t in scratch] + [
            dma((3 * HEADS + 9,)), dma((2, sp)), dma((2, sp)), dma((2 * nz,)), dma((tp,)), dma((tp,)), dma((tp,)),
            dma((2 * ny,)), dma((sp,)), dma((sp,)), dma((sp,)), dma((2 * nz,)), dma((tp,)),
            dma((ny, tp)), dma((sp, tp)), dma((sp, tp)), dma((sp, tp)), dma((nz + 1,)), dma((nz + 1,)),
        ],
        compiler_params=pltpu.CompilerParams(
            collective_id=0, has_side_effects=True, vmem_limit_bytes=VMEM_BYTES
        ),
    )(log_norm.T, keys, values, queries, attn_out, cotangent, source, w_query, w_key, w_value))


def scratch_of(sp, tp, queries, keys, source, w_query, w_value):
    rows, width = queries.shape
    rs, kw = keys.shape
    stack = (KV_HEADS, rows * HEADS // KV_HEADS, HEAD_DIM)
    flat = stack[:2] + (128,)
    return [
        ((2, tp, sp * rs, kw), BF16), (stack, BF16), (stack, BF16), (stack, BF16),
        (w_query.shape, BF16), (w_value.shape, BF16), (w_value.shape, BF16),
        ((sp,) + source.shape, BF16), ((sp,) + source.shape[::-1], BF16), (flat, F32), (flat, F32), (stack, F32), ((rows, width), BF16),
        ((sp, 2, rs, kw), BF16), ((sp, 2, rs, kw), BF16), ((sp, tp, 2, rs, kw), BF16),
    ]


def shards(sp, tp, *args):
    queries, _, _, _, keys, _, source, w_query, _, w_value = args
    scratch = scratch_of(sp, tp, queries, keys, source, w_query, w_value)
    size = sum(math.prod(s) * jnp.dtype(t).itemsize for s, t in scratch)
    fits = size * 2 < VMEM_BYTES and sp * keys.shape[0] == 128
    if fits and sp % CORES == 0 and tp == 4 * SIDE:
        return fused(sp, tp, scratch, *args)
    return plain(*args)


def plain(queries, attn_out, log_norm, cotangent, keys, values, source, w_query, w_key, w_value):
    single_precision = jnp.float32
    repeat = HEADS // KV_HEADS
    score_scale = 1.0 / math.sqrt(HEAD_DIM)
    rows = queries.shape[0]
    near_keys, near_values = (
        lax.all_gather(keys, "sp", axis=0, tiled=True),
        lax.all_gather(values, "sp", axis=0, tiled=True),
    )
    span = near_keys.shape[0]
    query_tensor4 = queries.reshape(rows, KV_HEADS, repeat, HEAD_DIM)
    output_gradient4 = cotangent.reshape(rows, KV_HEADS, repeat, HEAD_DIM)
    out4 = attn_out.reshape(rows, KV_HEADS, repeat, HEAD_DIM)
    shared_key_heads = near_keys.reshape(span, KV_HEADS, HEAD_DIM)
    shared_value_heads = near_values.reshape(span, KV_HEADS, HEAD_DIM)
    delta = jnp.sum(
        output_gradient4.astype(single_precision) * out4.astype(single_precision), axis=3
    )
    delta = jnp.transpose(delta, (1, 2, 0))[..., None]
    lse = jnp.transpose(log_norm.reshape(rows, KV_HEADS, repeat), (1, 2, 0))[..., None]
    logit_scores = (
        jnp.einsum(
            "znjk,wnk->njzw",
            query_tensor4,
            shared_key_heads,
            preferred_element_type=single_precision,
        )
        * score_scale
    )
    probs = jnp.exp(logit_scores - lse)
    probabilities16 = probs.astype(jnp.bfloat16)
    prob_gradient = jnp.einsum(
        "znjk,wnk->njzw",
        output_gradient4,
        shared_value_heads,
        preferred_element_type=single_precision,
    )
    score_gradient = (probs * (prob_gradient - delta)).astype(jnp.bfloat16)
    query_gradient_piece = (
        jnp.einsum(
            "wohn,nwb->hwob",
            score_gradient,
            shared_key_heads,
            preferred_element_type=single_precision,
        )
        * score_scale
    )
    query_gradient_piece = query_gradient_piece.reshape(rows, -1)
    key_gradient_piece = (
        jnp.einsum(
            "nkjv,jnka->vna", score_gradient, query_tensor4, preferred_element_type=single_precision
        )
        * score_scale
    )
    value_gradient_piece = jnp.einsum(
        "nkjv,jnka->vna", probabilities16, output_gradient4, preferred_element_type=single_precision
    )
    own_keys, own_values = (
        lax.psum_scatter(
            key_gradient_piece.reshape(span, -1).astype(jnp.bfloat16),
            "sp",
            scatter_dimension=0,
            tiled=True,
        ).astype(jnp.float32),
        lax.psum_scatter(
            value_gradient_piece.reshape(span, -1).astype(jnp.bfloat16),
            "sp",
            scatter_dimension=0,
            tiled=True,
        ).astype(jnp.float32),
    )
    stacked = jnp.concatenate(
        [own_keys.astype(jnp.bfloat16), own_values.astype(jnp.bfloat16)], axis=1
    )
    group = lax.all_gather(stacked, "tp", axis=0, tiled=True)
    weights = jnp.concatenate([w_key, w_value], axis=1)
    d_source = lax.dot_general(
        group, weights, (((1,), (1,)), ((), ())), preferred_element_type=single_precision
    ).astype(jnp.bfloat16)
    kv_width = w_value.shape[1]
    weight_term = lax.dot_general(
        source,
        group[:, kv_width:],
        (((0,), (0,)), ((), ())),
        preferred_element_type=single_precision,
    )
    d_wvalue = lax.psum(weight_term.astype(jnp.bfloat16), "sp").astype(jnp.float32)
    dq16 = lax.psum(query_gradient_piece, "tp").astype(jnp.bfloat16)
    d_target = lax.dot_general(
        dq16, w_query, (((1,), (1,)), ((), ())), preferred_element_type=single_precision
    ).astype(jnp.bfloat16)
    return (d_target, d_source, d_wvalue)


def solution(mesh):
    body = functools.partial(shards, mesh.shape["sp"], mesh.shape["tp"])
    in_specs = (
        P("sp", None),
        P("sp", None),
        P("sp", None),
        P("sp", None),
        P(("sp", "tp"), None),
        P(("sp", "tp"), None),
        P("sp", "tp"),
        P("tp", None),
        P("tp", None),
        P("tp", None),
    )
    out_specs = (P("sp", "tp"), P("sp", "tp"), P("tp", None))
    return jax.shard_map(body, mesh=mesh, in_specs=in_specs, out_specs=out_specs, check_vma=False)
```
